32 devices in a mesh: sp: 16 (over z, y, x), tp: 2 (over core).
Axes of the slice: x: 2, y: 2, z: 4, core: 2. Of those that a mesh axis runs over, the one named last changes fastest.
Arguments:
- tokens: bfloat16 [8192, 4096], P(('sp', 'tp')), may hold values from -6 to 6
- norm_gain: float32 [4096], replicated, may hold values from 0.5 to 1.5
- query_weight: bfloat16 [4096, 1024], P(None, 'tp'), may hold values from -0.09375 to 0.09375
- key_weight: bfloat16 [4096, 1024], P(None, 'tp'), may hold values from -0.09375 to 0.09375
- value_weight: bfloat16 [4096, 2048], P(None, 'tp'), may hold values from -0.09375 to 0.09375
- gate_weight: bfloat16 [4096, 2048], P(None, 'tp'), may hold values from -0.09375 to 0.09375
- decay_bias: float32 [1024], P('tp'), may hold values from -0.5 to 0.5
- head_gain: float32 [2048], P('tp'), may hold values from 0.5 to 1.5
- out_weight: bfloat16 [2048, 4096], P('tp'), may hold values from -0.125 to 0.125
Outputs:
- layer_out: bfloat16 [8192, 4096], P(('sp', 'tp'))
The draws below stay inside these ranges and needn't reach their ends.
All inputs are finite; a program needn't handle non-finite values.
Results may differ from the reference program's by a relative error of at most 0.015.
Values may be sent and summed in bfloat16 or wider, within the bound.
A program may use at most 192 MiB of HBM per device.

```python
import math
import jax
import jax.numpy as jnp
from jax import lax

D = 4096
HEADS = 8
HEAD_K = 128
HEAD_V = 256
BLOCK = 64
SEQ = 8192
KEY_DIM = 1024
VALUE_DIM = 2048


def level_of(own_key, dims, cuts, least, top_value):
    level, own = 1.0, jax.random.fold_in(own_key, 6)
    for axis_at, shards_of in cuts:
        steps = jnp.exp(jax.random.uniform(jax.random.fold_in(own, axis_at), (shards_of,), jnp.float32, least / len(cuts), top_value / len(cuts)))
        level = level * jnp.repeat(steps, dims[axis_at] // shards_of).reshape([-1 if axis == axis_at else 1 for axis in range(len(dims))])
    return level


def bell_draw(rng, extent, spread, reach, shards=(), kind=jnp.bfloat16):
    gain = level_of(rng, extent, shards, -0.22, 0.18) if shards else 1.0
    array = jax.random.normal(rng, extent, jnp.float32) * spread * gain
    return jnp.minimum(jnp.maximum(array, -reach), reach).astype(kind)


def setup_inputs(seed: int = 0) -> dict:
    key_list = jax.random.split(jax.random.key(seed), 10)
    tokens = bell_draw(key_list[0], (SEQ, D), 1.0, 6.0, ((0, 32),))
    norm_gain = jnp.clip(1.0 + 0.1 * jax.random.normal(key_list[1], (D,), jnp.float32), 0.5, 1.5)
    query_weight = bell_draw(key_list[2], (D, KEY_DIM), D ** -0.5, 0.09375, ((1, 2),))
    key_weight = bell_draw(key_list[3], (D, KEY_DIM), D ** -0.5, 0.09375, ((1, 2),))
    value_weight = bell_draw(key_list[4], (D, VALUE_DIM), D ** -0.5, 0.09375, ((1, 2),))
    gate_weight = bell_draw(key_list[5], (D, VALUE_DIM), D ** -0.5, 0.09375, ((1, 2),))
    decay_bias = jnp.clip(jax.random.uniform(key_list[6], (KEY_DIM,), jnp.float32, -0.5, 0.5) * level_of(key_list[6], (KEY_DIM,), ((0, 2),), -0.4, 0.0), -0.5, 0.5)
    head_gain = jnp.clip(1.0 + 0.1 * jax.random.normal(key_list[7], (VALUE_DIM,), jnp.float32), 0.5, 1.5)
    out_weight = bell_draw(key_list[8], (VALUE_DIM, D), VALUE_DIM ** -0.5, 0.125, ((0, 2),))
    return {"tokens": tokens, "norm_gain": norm_gain, "query_weight": query_weight, "key_weight": key_weight, "value_weight": value_weight, "gate_weight": gate_weight, "decay_bias": decay_bias, "head_gain": head_gain, "out_weight": out_weight}


epsilon = 1e-06
decay_power = 16.0
precise = lax.Precision.HIGHEST

def to_blocks(values, head_count, head_width):
    block_count = values.shape[0] // BLOCK
    return values.astype(jnp.float32).reshape(block_count, BLOCK, head_count, head_width).transpose(0, 2, 1, 3)

def reference(tokens, norm_gain, query_weight, key_weight, value_weight, gate_weight, decay_bias, head_gain, out_weight):
    inputs = tokens.astype(jnp.float32)
    row_scale = lax.rsqrt(lax.optimization_barrier(jnp.mean(inputs * inputs, axis=-1, keepdims=True)) + epsilon)
    normed = (inputs * row_scale * norm_gain.astype(jnp.float32)).astype(jnp.bfloat16)
    query_rows = jnp.dot(normed, query_weight, preferred_element_type=jnp.float32).astype(jnp.bfloat16)
    key_rows = jnp.dot(normed, key_weight, preferred_element_type=jnp.float32).astype(jnp.bfloat16)
    value_rows = jnp.dot(normed, value_weight, preferred_element_type=jnp.float32).astype(jnp.bfloat16)
    gate_input = jnp.dot(normed, gate_weight, preferred_element_type=jnp.float32).astype(jnp.bfloat16)
    logits = decay_bias.astype(jnp.float32) + math.log(SEQ / 8.0)
    log_decay = jnp.broadcast_to(jax.nn.log_sigmoid(logits) / decay_power, (SEQ, KEY_DIM))
    query_blocks = to_blocks(query_rows, HEADS, HEAD_K) * HEAD_K ** (-0.5)
    key_blocks = to_blocks(key_rows, HEADS, HEAD_K)
    value_blocks = to_blocks(value_rows, HEADS, HEAD_V)
    decay_blocks = to_blocks(log_decay, HEADS, HEAD_K)
    within = jnp.cumsum(decay_blocks, axis=2)
    block_end = within[:, :, -1:, :]
    query_in = query_blocks * jnp.exp(within)
    key_in = key_blocks * jnp.exp(-within)
    key_out = key_blocks * jnp.exp(block_end - within)
    causal = jnp.tril(jnp.ones((BLOCK, BLOCK), dtype=bool))
    scores = jnp.where(causal, jnp.einsum('nhid,nhjd->nhij', query_in, key_in, precision=precise), 0.0)
    local_out = jnp.einsum('nhij,nhjv->nhiv', scores, value_blocks, precision=precise)
    block_decay = jnp.exp(block_end[:, :, 0, :])

    def advance(carry_state, inputs_now):
        query_now, key_now, value_now, decay_now = inputs_now
        carried = jnp.einsum('hid,hdv->hiv', query_now, carry_state, precision=precise)
        carry_state = decay_now[..., None] * carry_state + jnp.einsum('hjd,hjv->hdv', key_now, value_now, precision=precise)
        return (carry_state, carried)
    start_state = jnp.zeros((HEADS, HEAD_K, HEAD_V), jnp.float32)
    _, carried_out = lax.scan(advance, start_state, (query_in, key_out, value_blocks, block_decay))
    mixed_heads = (local_out + carried_out).transpose(0, 2, 1, 3).reshape(SEQ, HEADS, HEAD_V)
    head_scale = lax.rsqrt(lax.optimization_barrier(jnp.mean(mixed_heads * mixed_heads, axis=-1, keepdims=True)) + epsilon)
    normed_heads = (mixed_heads * head_scale * head_gain.astype(jnp.float32).reshape(HEADS, HEAD_V)).reshape(SEQ, HEADS * HEAD_V)
    gated_rows = (normed_heads * jax.nn.silu(gate_input.astype(jnp.float32))).astype(jnp.bfloat16)
    return jnp.dot(gated_rows, out_weight, preferred_element_type=jnp.float32).astype(jnp.bfloat16)
```

```python
import functools
import math

import jax
import jax.numpy as jnp
from jax import lax
from jax.experimental import pallas as pl
from jax.experimental.pallas import tpu as pltpu
from jax.sharding import PartitionSpec as P

HEAD_K = 128
HEAD_V = 256

epsilon = 1e-06
decay_power = 16.0
MESH = pl.DeviceIdType.MESH
f32 = jnp.float32
bf16 = jnp.bfloat16
OUT_TILE = 512
VMEM_BYTES = 67_000_000


def nn(a, b):
    return jnp.dot(a, b, preferred_element_type=f32)


def nt(a, b):
    return lax.dot_general(a, b, (((1,), (1,)), ((), ())), preferred_element_type=f32)


def tn(a, b):
    return lax.dot_general(a, b, (((0,), (0,)), ((), ())), preferred_element_type=f32)


def kernel(
    sp_count,
    tokens,
    norm_gain,
    wq,
    wk,
    wv,
    wg,
    decay_bias,
    head_gain,
    wo,
    out,
    xn,
    w,
    wout,
    y,
    kin,
    qin,
    pv,
    gated,
    st_send,
    st_recv,
    tot_send,
    tot_recv,
    acc,
    c_send,
    c_recv,
    o_send,
    o_recv,
    o_buf,
    tok_sem,
    w_sem,
    wo_sem,
    tok_send,
    tok_recv,
    a_send,
    a_recv,
    b_send,
    b_recv,
    cs_send,
    cs_recv,
    os_send,
    os_recv,
    ob_sem,
):
    s = lax.axis_index("sp")
    c = lax.axis_index("tp")
    other = 1 - c
    half = tokens.shape[0]
    span = 2 * half
    width = wk.shape[1]
    heads = width // HEAD_K
    per = width // HEAD_V
    vtiles = wv.shape[1] // width
    inner = heads
    groups = sp_count // inner
    g = s // inner
    j = lax.rem(s, inner)

    own = pl.ds(pl.multiple_of(c * half, half), half)
    theirs = pl.ds(pl.multiple_of(other * half, half), half)

    def inner_dev(i):
        return {"sp": g * inner + i, "tp": c}

    def group_dev(k):
        return {"sp": k * inner + j, "tp": c}

    local_tok = pltpu.make_async_copy(tokens, xn.at[own], tok_sem)
    local_tok.start()
    sources = [wk.at[:, :]]
    sources += [wv.at[:, pl.ds(t * width, width)] for t in range(vtiles)]
    sources += [wq.at[:, :]]
    sources += [wg.at[:, pl.ds(t * width, width)] for t in range(vtiles)]
    count = len(sources)
    pltpu.make_async_copy(sources[0], w.at[0], w_sem.at[0]).start()

    barrier = pltpu.get_barrier_semaphore()
    pl.semaphore_signal(barrier, inc=1, device_id={"sp": s, "tp": other}, device_id_type=MESH)
    for d in range(1, inner):
        pl.semaphore_signal(
            barrier, inc=1, device_id=inner_dev(lax.rem(j + d, inner)), device_id_type=MESH
        )
    for d in range(1, groups):
        pl.semaphore_signal(
            barrier, inc=1, device_id=group_dev(lax.rem(g + d, groups)), device_id_type=MESH
        )
    pl.semaphore_wait(barrier, inner + groups - 1)

    send_tok = pltpu.make_async_remote_copy(
        src_ref=tokens,
        dst_ref=xn.at[own],
        send_sem=tok_send,
        recv_sem=tok_recv,
        device_id={"sp": s, "tp": other},
        device_id_type=MESH,
    )
    send_tok.start()
    for t in range(1, count):
        pltpu.make_async_copy(sources[t], w.at[t], w_sem.at[t]).start()
    wo_copy = pltpu.make_async_copy(wo, wout, wo_sem)
    wo_copy.start()

    chunk = 16

    def norm_rows(first):
        @pl.loop(0, half // chunk)
        def _(i):
            rows = pl.ds(pl.multiple_of(first + i * chunk, chunk), chunk)
            x = xn[rows, :].astype(f32)
            scale = lax.rsqrt(jnp.mean(x * x, axis=-1, keepdims=True) + epsilon)
            xn[rows, :] = (x * scale * norm_gain[...]).astype(bf16)

    def wait_w(t):
        pltpu.make_async_copy(wk, w.at[t], w_sem.at[t]).wait()

    local_tok.wait()
    norm_rows(c * half)
    wait_w(0)
    y[0, own, :] = nn(xn[own, :], w[0]).astype(bf16)
    send_tok.wait()
    norm_rows(other * half)
    y[0, theirs, :] = nn(xn[theirs, :], w[0]).astype(bf16)

    def project(t):
        wait_w(t)
        y[t] = nn(xn[...], w[t]).astype(bf16)

    @pl.loop(1, 1 + vtiles)
    def _(t):
        project(t)

    def log_decay_of(bias):
        return -jnp.log1p(jnp.exp(-(bias + math.log(sp_count * span / 8.0)))) / decay_power

    steps = (lax.broadcasted_iota(jnp.int32, (span, HEAD_K), 0) + 1).astype(f32)

    def column(row):
        half_tile = jnp.broadcast_to(row, (HEAD_K, HEAD_K)).T
        return jnp.concatenate([half_tile] * (HEAD_V // HEAD_K), axis=1)

    def value_of(h):
        return y[1 + h // per, :, pl.ds((h % per) * HEAD_V, HEAD_V)]

    for h in range(heads):
        keys = pl.ds(h * HEAD_K, HEAD_K)
        row = log_decay_of(decay_bias[pl.ds(h, 1), :])
        k_here = (y[0, :, keys].astype(f32) * jnp.exp(-row * steps)).astype(bf16)
        kin[:, keys] = k_here
        st_send[h] = (tn(k_here, value_of(h)) * column(jnp.exp(row * span))).astype(bf16)

    def copies(src, dst, ssem, rsem):
        made = []
        for d in range(1, inner):
            i = lax.rem(j + d, inner)
            made.append(
                pltpu.make_async_remote_copy(
                    src_ref=src.at[i],
                    dst_ref=dst.at[j],
                    send_sem=ssem.at[d - 1],
                    recv_sem=rsem.at[d - 1],
                    device_id=inner_dev(i),
                    device_id_type=MESH,
                )
            )
        return made

    a_copies = copies(st_send, st_recv, a_send, a_recv)
    for copy in a_copies:
        copy.start()
    st_recv[j] = st_send[j]

    @pl.loop(1 + vtiles, 3 + vtiles)
    def _(t):
        project(t)

    for copy in a_copies:
        copy.wait()
    mine = log_decay_of(decay_bias[pl.ds(j, 1), :])
    step_decay = column(jnp.exp(mine * span))
    total = st_recv[0].astype(f32)
    for i in range(1, inner):
        total = total * step_decay + st_recv[i].astype(f32)
    tot_send[...] = total.astype(bf16)

    def b_copy(d):
        return pltpu.make_async_remote_copy(
            src_ref=tot_send,
            dst_ref=tot_recv.at[d - 1],
            send_sem=b_send.at[d - 1],
            recv_sem=b_recv.at[d - 1],
            device_id=group_dev(lax.rem(g + d, groups)),
            device_id_type=MESH,
        )

    for d in range(1, groups):

        @pl.when(g + d < groups)
        def _():
            b_copy(d).start()

    @pl.loop(3 + vtiles, count)
    def _(t):
        project(t)

    for h in range(heads):
        keys = pl.ds(h * HEAD_K, HEAD_K)
        values = pl.ds(h * HEAD_V, HEAD_V)
        row = log_decay_of(decay_bias[pl.ds(h, 1), :])
        q_here = (
            y[1 + vtiles, :, keys].astype(f32) * (jnp.exp(row * steps) * HEAD_K ** (-0.5))
        ).astype(bf16)
        qin[:, keys] = q_here
        v_here = value_of(h)
        parts = 2
        rows = span // parts
        for p in range(parts):
            last = (p + 1) * rows
            scores = nt(q_here[p * rows : last], kin[pl.ds(0, last), keys])
            at = lax.broadcasted_iota(jnp.int32, scores.shape, 0) + p * rows
            to = lax.broadcasted_iota(jnp.int32, scores.shape, 1)
            scores = jnp.where(to <= at, scores, 0.0).astype(bf16)
            pv[pl.ds(p * rows, rows), values] = nn(scores, v_here[:last])

    acc[...] = jnp.zeros_like(acc)
    for d in range(1, groups):

        @pl.when(g >= d)
        def _():
            b_copy(d).wait_recv()
            far = column(jnp.exp(mine * (span * inner * (d - 1))))
            acc[...] += tot_recv[d - 1].astype(f32) * far

    carry = acc[...]
    c_send[0] = carry.astype(bf16)
    for i in range(1, inner):
        carry = carry * step_decay + st_recv[i - 1].astype(f32)
        c_send[i] = carry.astype(bf16)
    c_copies = copies(c_send, c_recv, cs_send, cs_recv)
    for copy in c_copies:
        copy.start()
    c_recv[j] = c_send[j]
    for copy in c_copies:
        copy.wait()

    for h in range(heads):
        keys = pl.ds(h * HEAD_K, HEAD_K)
        values = pl.ds(h * HEAD_V, HEAD_V)
        att = pv[:, values] + nn(qin[:, keys], c_recv[h])
        scale = lax.rsqrt(jnp.mean(att * att, axis=-1, keepdims=True) + epsilon)
        u = y[2 + vtiles + h // per, :, pl.ds((h % per) * HEAD_V, HEAD_V)].astype(f32)
        silu = u / (1.0 + jnp.exp(-u))
        gated[:, values] = (att * scale * head_gain[:, values] * silu).astype(bf16)

    tiles = wout.shape[1] // OUT_TILE

    def o_copy(t):
        return pltpu.make_async_remote_copy(
            src_ref=o_send.at[t],
            dst_ref=o_recv.at[t],
            send_sem=os_send.at[t],
            recv_sem=os_recv.at[t],
            device_id={"sp": s, "tp": other},
            device_id_type=MESH,
        )

    def out_copy(t):
        columns = pl.ds(pl.multiple_of(t * OUT_TILE, OUT_TILE), OUT_TILE)
        return pltpu.make_async_copy(o_buf.at[t], out.at[:, columns], ob_sem.at[t])

    wo_copy.wait()

    @pl.loop(0, tiles)
    def _(t):
        columns = pl.ds(pl.multiple_of(t * OUT_TILE, OUT_TILE), OUT_TILE)
        o_send[t] = nn(gated[theirs, :], wout[:, columns]).astype(bf16)
        o_copy(t).start()

    @pl.loop(0, tiles)
    def _(t):
        columns = pl.ds(pl.multiple_of(t * OUT_TILE, OUT_TILE), OUT_TILE)
        part = nn(gated[own, :], wout[:, columns])
        o_copy(t).wait()
        o_buf[t] = (part + o_recv[t].astype(f32)).astype(bf16)
        out_copy(t).start()

    @pl.loop(0, tiles)
    def _(t):
        out_copy(t).wait()

    for d in range(1, groups):

        @pl.when(g + d < groups)
        def _():
            b_copy(d).wait_send()


def per_device(sp_count, tokens, norm_gain, wq, wk, wv, wg, decay_bias, head_gain, wo):
    half, model = tokens.shape
    span = 2 * half
    width = wk.shape[1]
    vwidth = wv.shape[1]
    vtiles = vwidth // width
    heads = width // HEAD_K
    groups = sp_count // heads
    count = 2 + 2 * vtiles
    tiles = model // OUT_TILE
    state = (HEAD_K, HEAD_V)
    vm = pltpu.VMEM
    dma = pltpu.SemaphoreType.DMA
    hbm = pl.BlockSpec(memory_space=pltpu.HBM)
    vmem = pl.BlockSpec(memory_space=pltpu.VMEM)
    return pl.pallas_call(
        functools.partial(kernel, sp_count),
        out_shape=jax.ShapeDtypeStruct((half, model), bf16),
        in_specs=[hbm, vmem, hbm, hbm, hbm, hbm, vmem, vmem, hbm],
        out_specs=hbm,
        scratch_shapes=[
            vm((span, model), bf16),
            vm((count, model, width), bf16),
            vm((vwidth, model), bf16),
            vm((count, span, width), bf16),
            vm((span, width), bf16),
            vm((span, width), bf16),
            vm((span, vwidth), f32),
            vm((span, vwidth), bf16),
            vm((heads,) + state, bf16),
            vm((heads,) + state, bf16),
            vm(state, bf16),
            vm((groups,) + state, bf16),
            vm(state, f32),
            vm((heads,) + state, bf16),
            vm((heads,) + state, bf16),
            vm((tiles, half, OUT_TILE), bf16),
            vm((tiles, half, OUT_TILE), bf16),
            vm((tiles, half, OUT_TILE), bf16),
            dma,
            dma((count,)),
            dma,
            dma,
            dma,
            dma((heads,)),
            dma((heads,)),
            dma((groups,)),
            dma((groups,)),
            dma((heads,)),
            dma((heads,)),
            dma((tiles,)),
            dma((tiles,)),
            dma((tiles,)),
        ],
        compiler_params=pltpu.CompilerParams(
            collective_id=0, has_side_effects=True, vmem_limit_bytes=VMEM_BYTES
        ),
    )(
        tokens,
        norm_gain.reshape(1, model),
        wq,
        wk,
        wv,
        wg,
        decay_bias.reshape(heads, HEAD_K),
        head_gain.reshape(1, vwidth),
        wo,
    )


def solution(mesh):
    return jax.shard_map(
        functools.partial(per_device, mesh.shape["sp"]),
        mesh=mesh,
        in_specs=(
            P(("sp", "tp"), None),
            P(),
            P(None, "tp"),
            P(None, "tp"),
            P(None, "tp"),
            P(None, "tp"),
            P("tp"),
            P("tp"),
            P("tp", None),
        ),
        out_specs=P(("sp", "tp"), None),
        check_vma=False,
    )
```

```python
import functools
import math

import jax
import jax.numpy as jnp
from jax import lax
from jax.experimental import pallas as pl
from jax.experimental.pallas import tpu as pltpu
from jax.sharding import PartitionSpec as P

HEAD_K = 128
HEAD_V = 256

epsilon = 1e-06
decay_power = 16.0
MESH = pl.DeviceIdType.MESH
f32 = jnp.float32
bf16 = jnp.bfloat16
OUT_TILE = 512
VMEM_BYTES = 67_000_000


def nn(a, b):
    return jnp.dot(a, b, preferred_element_type=f32)


def nt(a, b):
    return lax.dot_general(a, b, (((1,), (1,)), ((), ())), preferred_element_type=f32)


def tn(a, b):
    return lax.dot_general(a, b, (((0,), (0,)), ((), ())), preferred_element_type=f32)


def kernel(
    sp_count,
    tokens,
    norm_gain,
    wq,
    wk,
    wv,
    wg,
    decay_bias,
    head_gain,
    wo,
    out,
    xn,
    w,
    wout,
    y,
    kin,
    qin,
    pv,
    gated,
    st_send,
    st_recv,
    tot_send,
    tot_recv,
    acc,
    c_send,
    c_recv,
    o_send,
    o_recv,
    o_buf,
    tok_sem,
    w_sem,
    wo_sem,
    tok_send,
    tok_recv,
    a_send,
    a_recv,
    b_send,
    b_recv,
    cs_send,
    cs_recv,
    os_send,
    os_recv,
    ob_sem,
):
    s = lax.axis_index("sp")
    c = lax.axis_index("tp")
    other = 1 - c
    half = tokens.shape[0]
    span = 2 * half
    width = wk.shape[1]
    heads = width // HEAD_K
    per = width // HEAD_V
    vtiles = wv.shape[1] // width
    inner = heads
    groups = sp_count // inner
    g = s // inner
    j = lax.rem(s, inner)

    own = pl.ds(pl.multiple_of(c * half, half), half)
    theirs = pl.ds(pl.multiple_of(other * half, half), half)

    def inner_dev(i):
        return {"sp": g * inner + i, "tp": c}

    def group_dev(k):
        return {"sp": k * inner + j, "tp": c}

    local_tok = pltpu.make_async_copy(tokens, xn.at[own], tok_sem)
    local_tok.start()
    sources = [wk.at[:, :]]
    sources += [wv.at[:, pl.ds(t * width, width)] for t in range(vtiles)]
    sources += [wq.at[:, :]]
    sources += [wg.at[:, pl.ds(t * width, width)] for t in range(vtiles)]
    count = len(sources)
    pltpu.make_async_copy(sources[0], w.at[0], w_sem.at[0]).start()

    barrier = pltpu.get_barrier_semaphore()
    pl.semaphore_signal(barrier, inc=1, device_id={"sp": s, "tp": other}, device_id_type=MESH)
    for d in range(1, inner):
        pl.semaphore_signal(
            barrier, inc=1, device_id=inner_dev(lax.rem(j + d, inner)), device_id_type=MESH
        )
    for d in range(1, groups):
        pl.semaphore_signal(
            barrier, inc=1, device_id=group_dev(lax.rem(g + d, groups)), device_id_type=MESH
        )
    pl.semaphore_wait(barrier, inner + groups - 1)

    send_tok = pltpu.make_async_remote_copy(
        src_ref=tokens,
        dst_ref=xn.at[own],
        send_sem=tok_send,
        recv_sem=tok_recv,
        device_id={"sp": s, "tp": other},
        device_id_type=MESH,
    )
    send_tok.start()
    wo_copy = pltpu.make_async_copy(wo, wout, wo_sem)
    fetches = [pltpu.make_async_copy(sources[t], w.at[t], w_sem.at[t]) for t in range(count)]
    fetches.append(wo_copy)

    chunk = 16

    def norm_rows(first):
        @pl.loop(0, half // chunk)
        def _(i):
            rows = pl.ds(pl.multiple_of(first + i * chunk, chunk), chunk)
            x = xn[rows, :].astype(f32)
            scale = lax.rsqrt(jnp.mean(x * x, axis=-1, keepdims=True) + epsilon)
            xn[rows, :] = (x * scale * norm_gain[...]).astype(bf16)

    def wait_w(t):
        pltpu.make_async_copy(wk, w.at[t], w_sem.at[t]).wait()

    local_tok.wait()
    fetches[1].start()
    norm_rows(c * half)
    wait_w(0)
    fetches[2].start()
    y[0, own, :] = nn(xn[own, :], w[0]).astype(bf16)
    send_tok.wait()
    norm_rows(other * half)
    y[0, theirs, :] = nn(xn[theirs, :], w[0]).astype(bf16)

    def project(t):
        wait_w(t)
        for k in range(3, count + 1):

            @pl.when(t + 2 == k)
            def _():
                fetches[k].start()

        y[t] = nn(xn[...], w[t]).astype(bf16)

    @pl.loop(1, 1 + vtiles)
    def _(t):
        project(t)

    def log_decay_of(bias):
        return -jnp.log1p(jnp.exp(-(bias + math.log(sp_count * span / 8.0)))) / decay_power

    steps = (lax.broadcasted_iota(jnp.int32, (span, HEAD_K), 0) + 1).astype(f32)

    def column(row):
        half_tile = jnp.broadcast_to(row, (HEAD_K, HEAD_K)).T
        return jnp.concatenate([half_tile] * (HEAD_V // HEAD_K), axis=1)

    def value_of(h):
        return y[1 + h // per, :, pl.ds((h % per) * HEAD_V, HEAD_V)]

    for h in range(heads):
        keys = pl.ds(h * HEAD_K, HEAD_K)
        row = log_decay_of(decay_bias[pl.ds(h, 1), :])
        k_here = (y[0, :, keys].astype(f32) * jnp.exp(-row * steps)).astype(bf16)
        kin[:, keys] = k_here
        st_send[h] = (tn(k_here, value_of(h)) * column(jnp.exp(row * span))).astype(bf16)

    def copies(src, dst, ssem, rsem):
        made = []
        for d in range(1, inner):
            i = lax.rem(j + d, inner)
            made.append(
                pltpu.make_async_remote_copy(
                    src_ref=src.at[i],
                    dst_ref=dst.at[j],
                    send_sem=ssem.at[d - 1],
                    recv_sem=rsem.at[d - 1],
                    device_id=inner_dev(i),
                    device_id_type=MESH,
                )
            )
        return made

    a_copies = copies(st_send, st_recv, a_send, a_recv)
    for copy in a_copies:
        copy.start()
    st_recv[j] = st_send[j]

    @pl.loop(1 + vtiles, 3 + vtiles)
    def _(t):
        project(t)

    for copy in a_copies:
        copy.wait()
    mine = log_decay_of(decay_bias[pl.ds(j, 1), :])
    step_decay = column(jnp.exp(mine * span))
    total = st_recv[0].astype(f32)
    for i in range(1, inner):
        total = total * step_decay + st_recv[i].astype(f32)
    tot_send[...] = total.astype(bf16)

    def b_copy(d):
        return pltpu.make_async_remote_copy(
            src_ref=tot_send,
            dst_ref=tot_recv.at[d - 1],
            send_sem=b_send.at[d - 1],
            recv_sem=b_recv.at[d - 1],
            device_id=group_dev(lax.rem(g + d, groups)),
            device_id_type=MESH,
        )

    for d in range(1, groups):

        @pl.when(g + d < groups)
        def _():
            b_copy(d).start()

    @pl.loop(3 + vtiles, count)
    def _(t):
        project(t)

    for h in range(heads):
        keys = pl.ds(h * HEAD_K, HEAD_K)
        values = pl.ds(h * HEAD_V, HEAD_V)
        row = log_decay_of(decay_bias[pl.ds(h, 1), :])
        q_here = (
            y[1 + vtiles, :, keys].astype(f32) * (jnp.exp(row * steps) * HEAD_K ** (-0.5))
        ).astype(bf16)
        qin[:, keys] = q_here
        v_here = value_of(h)
        parts = 2
        rows = span // parts
        for p in range(parts):
            last = (p + 1) * rows
            scores = nt(q_here[p * rows : last], kin[pl.ds(0, last), keys])
            at = lax.broadcasted_iota(jnp.int32, scores.shape, 0) + p * rows
            to = lax.broadcasted_iota(jnp.int32, scores.shape, 1)
            scores = jnp.where(to <= at, scores, 0.0).astype(bf16)
            pv[pl.ds(p * rows, rows), values] = nn(scores, v_here[:last])

    acc[...] = jnp.zeros_like(acc)
    for d in range(1, groups):

        @pl.when(g >= d)
        def _():
            b_copy(d).wait_recv()
            far = column(jnp.exp(mine * (span * inner * (d - 1))))
            acc[...] += tot_recv[d - 1].astype(f32) * far

    carry = acc[...]
    c_send[0] = carry.astype(bf16)
    for i in range(1, inner):
        carry = carry * step_decay + st_recv[i - 1].astype(f32)
        c_send[i] = carry.astype(bf16)
    c_copies = copies(c_send, c_recv, cs_send, cs_recv)
    for copy in c_copies:
        copy.start()
    c_recv[j] = c_send[j]
    for copy in c_copies:
        copy.wait()

    for h in range(heads):
        keys = pl.ds(h * HEAD_K, HEAD_K)
        values = pl.ds(h * HEAD_V, HEAD_V)
        att = pv[:, values] + nn(qin[:, keys], c_recv[h])
        scale = lax.rsqrt(jnp.mean(att * att, axis=-1, keepdims=True) + epsilon)
        u = y[2 + vtiles + h // per, :, pl.ds((h % per) * HEAD_V, HEAD_V)].astype(f32)
        silu = u / (1.0 + jnp.exp(-u))
        gated[:, values] = (att * scale * head_gain[:, values] * silu).astype(bf16)

    tiles = wout.shape[1] // OUT_TILE

    def o_copy(t):
        return pltpu.make_async_remote_copy(
            src_ref=o_send.at[t],
            dst_ref=o_recv.at[t],
            send_sem=os_send.at[t],
            recv_sem=os_recv.at[t],
            device_id={"sp": s, "tp": other},
            device_id_type=MESH,
        )

    def out_copy(t):
        columns = pl.ds(pl.multiple_of(t * OUT_TILE, OUT_TILE), OUT_TILE)
        return pltpu.make_async_copy(o_buf.at[t], out.at[:, columns], ob_sem.at[t])

    wo_copy.wait()

    @pl.loop(0, tiles)
    def _(t):
        columns = pl.ds(pl.multiple_of(t * OUT_TILE, OUT_TILE), OUT_TILE)
        o_send[t] = nn(gated[theirs, :], wout[:, columns]).astype(bf16)
        o_copy(t).start()

    @pl.loop(0, tiles)
    def _(t):
        columns = pl.ds(pl.multiple_of(t * OUT_TILE, OUT_TILE), OUT_TILE)
        part = nn(gated[own, :], wout[:, columns])
        o_copy(t).wait()
        o_buf[t] = (part + o_recv[t].astype(f32)).astype(bf16)
        out_copy(t).start()

    @pl.loop(0, tiles)
    def _(t):
        out_copy(t).wait()

    for d in range(1, groups):

        @pl.when(g + d < groups)
        def _():
            b_copy(d).wait_send()


def per_device(sp_count, tokens, norm_gain, wq, wk, wv, wg, decay_bias, head_gain, wo):
    half, model = tokens.shape
    span = 2 * half
    width = wk.shape[1]
    vwidth = wv.shape[1]
    vtiles = vwidth // width
    heads = width // HEAD_K
    groups = sp_count // heads
    count = 2 + 2 * vtiles
    tiles = model // OUT_TILE
    state = (HEAD_K, HEAD_V)
    vm = pltpu.VMEM
    dma = pltpu.SemaphoreType.DMA
    hbm = pl.BlockSpec(memory_space=pltpu.HBM)
    vmem = pl.BlockSpec(memory_space=pltpu.VMEM)
    return pl.pallas_call(
        functools.partial(kernel, sp_count),
        out_shape=jax.ShapeDtypeStruct((half, model), bf16),
        in_specs=[hbm, vmem, hbm, hbm, hbm, hbm, vmem, vmem, hbm],
        out_specs=hbm,
        scratch_shapes=[
            vm((span, model), bf16),
            vm((count, model, width), bf16),
            vm((vwidth, model), bf16),
            vm((count, span, width), bf16),
            vm((span, width), bf16),
            vm((span, width), bf16),
            vm((span, vwidth), f32),
            vm((span, vwidth), bf16),
            vm((heads,) + state, bf16),
            vm((heads,) + state, bf16),
            vm(state, bf16),
            vm((groups,) + state, bf16),
            vm(state, f32),
            vm((heads,) + state, bf16),
            vm((heads,) + state, bf16),
            vm((tiles, half, OUT_TILE), bf16),
            vm((tiles, half, OUT_TILE), bf16),
            vm((tiles, half, OUT_TILE), bf16),
            dma,
            dma((count,)),
            dma,
            dma,
            dma,
            dma((heads,)),
            dma((heads,)),
            dma((groups,)),
            dma((groups,)),
            dma((heads,)),
            dma((heads,)),
            dma((tiles,)),
            dma((tiles,)),
            dma((tiles,)),
        ],
        compiler_params=pltpu.CompilerParams(
            collective_id=0, has_side_effects=True, vmem_limit_bytes=VMEM_BYTES
        ),
    )(
        tokens,
        norm_gain.reshape(1, model),
        wq,
        wk,
        wv,
        wg,
        decay_bias.reshape(heads, HEAD_K),
        head_gain.reshape(1, vwidth),
        wo,
    )


def solution(mesh):
    return jax.shard_map(
        functools.partial(per_device, mesh.shape["sp"]),
        mesh=mesh,
        in_specs=(
            P(("sp", "tp"), None),
            P(),
            P(None, "tp"),
            P(None, "tp"),
            P(None, "tp"),
            P(None, "tp"),
            P("tp"),
            P("tp"),
            P("tp", None),
        ),
        out_specs=P(("sp", "tp"), None),
        check_vma=False,
    )
```
